512 devices in a mesh: rep: 2 (over z_hi), fs: 32 (over z_lo, y), tp: 8 (over x, core).
Axes of the slice: x: 4, y: 4, z: 16 (z_hi: 2, z_lo: 8; z = z_hi * 8 + z_lo), core: 2. Of those that a mesh axis runs over, the one named last changes fastest.
Arguments:
- input_activation_entries: bfloat16 [24576, 2048], P(('rep', 'fs')), may hold values from -6 to 6
- premixing_rescale_factor: float32 [2048], replicated, may hold values from 0.1 to 1.9
- probe_weight_table: float32 [2048, 1024], P('fs', 'tp'), may hold values from -0.125 to 0.125
- probe_factor_list: float32 [1024], P('tp'), may hold values from 0.5 to 2
- lookup_weight_table: float32 [2048, 1024], P('fs', 'tp'), may hold values from -0.125 to 0.125
- lookup_factor_list: float32 [1024], P('tp'), may hold values from 0.5 to 2
- forget_weight_table: float32 [2048, 1024], P('fs', 'tp'), may hold values from -0.125 to 0.125
- forget_factor_list: float32 [1024], P('tp'), may hold values from 1 to 8
- forget_shift_term: float32 [1024], P('tp'), may hold values from -3 to 7
- extra_forget_logs: float32 [24576, 8], P(('rep', 'fs'), 'tp'), may hold values from -0.7 to 0
- content_weight_table: float32 [2048, 2048], P('fs', 'tp'), may hold values from -0.125 to 0.125
- content_factor_list: float32 [2048], P('tp'), may hold values from 0.5 to 2
- filter_weight_table: float32 [2048, 2048], P('fs', 'tp'), may hold values from -0.125 to 0.125
- filter_factor_list: float32 [2048], P('tp'), may hold values from 0.5 to 2
- per_group_rescale_factor: float32 [2048], P('tp'), may hold values from 0.1 to 1.9
- emission_weight_table: float32 [2048, 2048], P('tp', 'fs'), may hold values from -0.125 to 0.125
- emission_factor_list: float32 [2048], P('fs'), may hold values from 0.5 to 2
- perceptron_prenorm_factor: float32 [2048], replicated, may hold values from 0.1 to 1.9
- raising_weight_table: float32 [2048, 8192], P('fs', 'tp'), may hold values from -0.125 to 0.125
- raising_factor_list: float32 [8192], P('tp'), may hold values from 0.5 to 2
- lowering_weight_table: float32 [8192, 2048], P('tp', 'fs'), may hold values from -0.0625 to 0.0625
- lowering_factor_list: float32 [2048], P('fs'), may hold values from 0.5 to 2
Outputs:
- layer_out: bfloat16 [24576, 2048], P(('rep', 'fs'))
The draws below stay inside these ranges and needn't reach their ends.
All inputs are finite; a program needn't handle non-finite values.
Results may differ from the reference program's by a relative error of at most 0.02.
Values may be sent and summed in bfloat16 or wider, within the bound.
No kernel may reach another device: no remote copies, remote signals or barrier semaphores. Data moves between devices by JAX's collectives and lax.ppermute only.
A program may use at most 64 MiB of HBM per device.

```python
import math
import jax
import jax.numpy as jnp
from jax import lax

D = 2048
HEADS = 8
LOOKUP_FEATURES = 128
FF = 8192
BLOCK = 64
TOK_DEV = 384
KW = 1024
VW = 2048
TOKENS = 24576
N_TP = 8


def draw_forget_shift_term(key, part):
    head_key, slow_key, fast_key = jax.random.split(key, 3)
    odds = 2
    fast_head = jax.random.randint(head_key, (HEADS,), 0, odds) == 0
    fast_channel = jnp.repeat(fast_head, LOOKUP_FEATURES)
    slow_value = jax.random.uniform(slow_key, (KW,), jnp.float32, 5.0, 7.0)
    fast_value = jax.random.uniform(fast_key, (KW,), jnp.float32, -3.0, -1.0)
    return jnp.where(fast_channel, fast_value, slow_value)


def draw_extra_forget_logs(key, part):
    rate_key, place_key, depth_key = jax.random.split(key, 3)
    blocks = TOKENS // BLOCK
    lowest = 0.0001
    rates = jnp.exp(jax.random.uniform(rate_key, (blocks, HEADS), jnp.float32, jnp.log(lowest), jnp.log(0.003)))
    base = -jnp.repeat(rates, BLOCK, axis=0)
    hits = jax.random.randint(place_key, (TOKENS, HEADS), 0, TOK_DEV) < 3
    depth = jnp.log(jax.random.uniform(depth_key, (TOKENS, HEADS), jnp.float32, 0.5, 0.8))
    return base + jnp.where(hits, depth, 0.0)


def levels(key, extent, cuts, least, largest):
    def one(position, shards_of):
        steps = jax.random.uniform(jax.random.fold_in(jax.random.fold_in(key, 6), position), (shards_of,), jnp.float32, least / len(cuts), largest / len(cuts))
        return jnp.repeat(jnp.exp(steps), extent[position] // shards_of).reshape((-1,) + (1,) * (len(extent) - position - 1))

    level = one(*cuts[0])
    for cut in cuts[1:]:
        level = level * one(*cut)
    return level


def noise(own_key, extent, scale, reach, shards=(), held_as=jnp.bfloat16):
    factor_of = levels(own_key, extent, shards, -0.22, 0.18) if shards else 1.0
    array = jax.random.normal(own_key, extent, jnp.float32) * scale * factor_of
    return jnp.minimum(jnp.maximum(array, -reach), reach).astype(held_as)


def setup_inputs(seed: int = 0) -> dict:
    key_of = jax.random.split(jax.random.key(seed), 23)
    input_activation_entries = noise(key_of[0], (TOKENS, D), 1.0, 6.0, ((0, 64),))
    premixing_rescale_factor = jnp.clip(1.0 + 0.18 * jax.random.normal(key_of[1], (D,), jnp.float32), 0.1, 1.9)
    probe_weight_table = noise(key_of[2], (D, KW), D ** -0.5, 0.125, ((0, 32), (1, 8)), jnp.float32)
    probe_factor_list = jnp.clip(jnp.exp(math.log(2.0) - 1.3862944 * jax.random.uniform(key_of[3], (KW,), jnp.float32) ** levels(key_of[3], (KW,), ((0, 8),), -0.2, 0.2)), 0.5, 2.0)
    lookup_weight_table = noise(key_of[4], (D, KW), D ** -0.5, 0.125, ((0, 32), (1, 8)), jnp.float32)
    lookup_factor_list = jnp.clip(jnp.exp(math.log(2.0) - 1.3862944 * jax.random.uniform(key_of[5], (KW,), jnp.float32) ** levels(key_of[5], (KW,), ((0, 8),), -0.2, 0.2)), 0.5, 2.0)
    forget_weight_table = noise(key_of[6], (D, KW), D ** -0.5, 0.125, ((0, 32), (1, 8)), jnp.float32)
    forget_factor_list = jnp.clip(jnp.exp(math.log(8.0) - 2.0794415 * jax.random.uniform(key_of[7], (KW,), jnp.float32) ** levels(key_of[7], (KW,), ((0, 8),), -0.2, 0.2)), 1.0, 8.0)
    forget_shift_term = draw_forget_shift_term(jax.random.fold_in(key_of[22], 71), 0)
    extra_forget_logs = draw_extra_forget_logs(jax.random.fold_in(key_of[22], 71), 0)
    content_weight_table = noise(key_of[10], (D, VW), D ** -0.5, 0.125, ((0, 32), (1, 8)), jnp.float32)
    content_factor_list = jnp.clip(jnp.exp(math.log(2.0) - 1.3862944 * jax.random.uniform(key_of[11], (VW,), jnp.float32) ** levels(key_of[11], (VW,), ((0, 8),), -0.2, 0.2)), 0.5, 2.0)
    filter_weight_table = noise(key_of[12], (D, VW), D ** -0.5, 0.125, ((0, 32), (1, 8)), jnp.float32)
    filter_factor_list = jnp.clip(jnp.exp(math.log(2.0) - 1.3862944 * jax.random.uniform(key_of[13], (VW,), jnp.float32) ** levels(key_of[13], (VW,), ((0, 8),), -0.2, 0.2)), 0.5, 2.0)
    per_group_rescale_factor = jnp.clip(1.0 + 0.18 * jax.random.normal(key_of[14], (VW,), jnp.float32), 0.1, 1.9)
    emission_weight_table = noise(key_of[15], (VW, D), VW ** -0.5, 0.125, ((0, 8), (1, 32)), jnp.float32)
    emission_factor_list = jnp.clip(jnp.exp(math.log(2.0) - 1.3862944 * jax.random.uniform(key_of[16], (D,), jnp.float32) ** levels(key_of[16], (D,), ((0, 32),), -0.2, 0.2)), 0.5, 2.0)
    perceptron_prenorm_factor = jnp.clip(1.0 + 0.18 * jax.random.normal(key_of[17], (D,), jnp.float32), 0.1, 1.9)
    raising_weight_table = noise(key_of[18], (D, FF), D ** -0.5, 0.125, ((0, 32), (1, 8)), jnp.float32)
    raising_factor_list = jnp.clip(jnp.exp(math.log(2.0) - 1.3862944 * jax.random.uniform(key_of[19], (FF,), jnp.float32) ** levels(key_of[19], (FF,), ((0, 8),), -0.2, 0.2)), 0.5, 2.0)
    lowering_weight_table = noise(key_of[20], (FF, D), FF ** -0.5, 0.0625, ((0, 8), (1, 32)), jnp.float32)
    lowering_factor_list = jnp.clip(jnp.exp(math.log(2.0) - 1.3862944 * jax.random.uniform(key_of[21], (D,), jnp.float32) ** levels(key_of[21], (D,), ((0, 32),), -0.2, 0.2)), 0.5, 2.0)
    return {"input_activation_entries": input_activation_entries, "premixing_rescale_factor": premixing_rescale_factor, "probe_weight_table": probe_weight_table, "probe_factor_list": probe_factor_list, "lookup_weight_table": lookup_weight_table, "lookup_factor_list": lookup_factor_list, "forget_weight_table": forget_weight_table, "forget_factor_list": forget_factor_list, "forget_shift_term": forget_shift_term, "extra_forget_logs": extra_forget_logs, "content_weight_table": content_weight_table, "content_factor_list": content_factor_list, "filter_weight_table": filter_weight_table, "filter_factor_list": filter_factor_list, "per_group_rescale_factor": per_group_rescale_factor, "emission_weight_table": emission_weight_table, "emission_factor_list": emission_factor_list, "perceptron_prenorm_factor": perceptron_prenorm_factor, "raising_weight_table": raising_weight_table, "raising_factor_list": raising_factor_list, "lowering_weight_table": lowering_weight_table, "lowering_factor_list": lowering_factor_list}


epsilon = 1e-06
filter_rescaled_entries = 16.0
highest = lax.Precision.HIGHEST

def rms_rows(matrix, gain):
    matrix = matrix.astype(jnp.float32)
    return matrix * lax.rsqrt(lax.optimization_barrier(jnp.mean(matrix * matrix, axis=-1, keepdims=True)) + epsilon) * gain

def recur_head(queries, keys_in, vals, forget_log_rate):
    length = queries.shape[0]
    blocks = length // BLOCK

    def to_blocks(tensor):
        return tensor.astype(jnp.float32).reshape(blocks, BLOCK, tensor.shape[-1])
    causal = jnp.tril(jnp.ones((BLOCK, BLOCK), dtype=bool))[:, :, None]

    def advance(memory, inputs):
        query_block, key_block, value_block, decay_block = inputs
        cumulative = jnp.cumsum(decay_block, axis=0)
        spread = cumulative[:, None, :] - cumulative[None, :, :]
        weights = jnp.exp(jnp.where(causal, spread, -jnp.inf))
        scores = jnp.einsum('tc,sc,tsc->ts', query_block, key_block, weights, precision=highest)
        within = jnp.dot(scores, value_block, precision=highest)
        carried = jnp.dot(query_block * jnp.exp(cumulative), memory, precision=highest)
        closing = cumulative[-1]
        scaled_keys = key_block * jnp.exp(closing[None, :] - cumulative)
        memory = jnp.exp(closing)[:, None] * memory + jnp.dot(scaled_keys.T, value_block, precision=highest)
        return (memory, within + carried)
    initial = jnp.zeros((queries.shape[-1], vals.shape[-1]), jnp.float32)
    _, outputs = lax.scan(advance, initial, (to_blocks(queries), to_blocks(keys_in), to_blocks(vals), to_blocks(forget_log_rate)))
    return outputs.reshape(length, vals.shape[-1])

def per_group_mixing_values(probe_mapped_entries, lookup_mapped_entries, forget_mapped_entries, content_mapped_entries, filter_mapped_entries, forget_shift_term, extra_forget_logs, per_group_rescale_factor):
    group_count_total = extra_forget_logs.shape[-1]
    queries = (jax.nn.silu(probe_mapped_entries) * LOOKUP_FEATURES ** (-0.5)).astype(jnp.bfloat16)
    keyed = jax.nn.silu(lookup_mapped_entries).astype(jnp.bfloat16)
    valued = jax.nn.silu(content_mapped_entries).astype(jnp.bfloat16)
    forget_log_rate = jax.nn.log_sigmoid(forget_mapped_entries + forget_shift_term) / filter_rescaled_entries + jnp.repeat(extra_forget_logs, LOOKUP_FEATURES, axis=1)

    def by_head(tensor):
        return tensor.reshape(tensor.shape[0], group_count_total, -1).transpose(1, 0, 2)
    outputs = jax.vmap(recur_head)(by_head(queries), by_head(keyed), by_head(valued), by_head(forget_log_rate))
    outputs = outputs * lax.rsqrt(lax.optimization_barrier(jnp.mean(outputs * outputs, axis=-1, keepdims=True)) + epsilon)
    merged = outputs.transpose(1, 0, 2).reshape(outputs.shape[1], -1)
    return (merged * per_group_rescale_factor * jax.nn.silu(filter_mapped_entries)).astype(jnp.bfloat16)

def grouped_sum(rows, weight, scale):
    rows_per = weight.shape[0] // N_TP
    running = jnp.zeros((rows.shape[0], weight.shape[1]), jnp.float32)
    for member in range(N_TP):
        piece = jnp.dot(rows[:, member * rows_per:(member + 1) * rows_per], weight[member * rows_per:(member + 1) * rows_per].astype(jnp.bfloat16), preferred_element_type=jnp.float32) * scale
        rounded = lax.optimization_barrier(piece.astype(jnp.bfloat16))
        running = running + rounded.astype(jnp.float32)
    return running

def reference(input_activation_entries, premixing_rescale_factor, probe_weight_table, probe_factor_list, lookup_weight_table, lookup_factor_list, forget_weight_table, forget_factor_list, forget_shift_term, extra_forget_logs, content_weight_table, content_factor_list, filter_weight_table, filter_factor_list, per_group_rescale_factor, emission_weight_table, emission_factor_list, perceptron_prenorm_factor, raising_weight_table, raising_factor_list, lowering_weight_table, lowering_factor_list):
    normed = rms_rows(input_activation_entries, premixing_rescale_factor).astype(jnp.bfloat16)

    def project(weight, scale):
        return jnp.dot(normed, weight.astype(jnp.bfloat16), preferred_element_type=jnp.float32) * scale
    probe_mapped_entries = project(probe_weight_table, probe_factor_list)
    lookup_mapped_entries = project(lookup_weight_table, lookup_factor_list)
    forget_mapped_entries = project(forget_weight_table, forget_factor_list)
    content_mapped_entries = project(content_weight_table, content_factor_list)
    filter_mapped_entries = project(filter_weight_table, filter_factor_list)
    seq_count = input_activation_entries.shape[0] // TOK_DEV

    def batched_by_stream(tensor):
        return tensor.reshape(seq_count, TOK_DEV, tensor.shape[-1])

    def per_stream_layout(pieces):
        return per_group_mixing_values(pieces[0], pieces[1], pieces[2], pieces[3], pieces[4], forget_shift_term, pieces[5], per_group_rescale_factor)
    mixing_product = lax.map(per_stream_layout, (batched_by_stream(probe_mapped_entries), batched_by_stream(lookup_mapped_entries), batched_by_stream(forget_mapped_entries), batched_by_stream(content_mapped_entries), batched_by_stream(filter_mapped_entries), batched_by_stream(extra_forget_logs)))
    mixing_product = mixing_product.reshape(input_activation_entries.shape[0], -1)
    mix_sum = grouped_sum(mixing_product, emission_weight_table, emission_factor_list)
    residual = (input_activation_entries.astype(jnp.float32) + mix_sum).astype(jnp.bfloat16)
    normed_mlp = rms_rows(residual, perceptron_prenorm_factor).astype(jnp.bfloat16)
    lifted = jnp.dot(normed_mlp, raising_weight_table.astype(jnp.bfloat16), preferred_element_type=jnp.float32) * raising_factor_list
    hidden = jnp.square(jax.nn.relu(lifted)).astype(jnp.bfloat16)
    mlp_sum = grouped_sum(hidden, lowering_weight_table, lowering_factor_list)
    return (residual.astype(jnp.float32) + mlp_sum).astype(jnp.bfloat16)
```

```python
import jax
import jax.numpy as jnp
import numpy as np
from jax import lax
from jax.experimental import pallas as pl
from jax.experimental.pallas import tpu as pltpu
from jax.sharding import PartitionSpec as P

EPS = 1e-06
BLOCK = 64
HALF = 64
ROWS = 384
D = 2048
BF = jnp.bfloat16
F32 = jnp.float32
HI = lax.Precision.HIGHEST
OFFSETS = (0, -1, 1, -2, 2, -3, 3, 4)
LEVELS = (32, 16, 8, 4, 2, 1)
ZY = ("rep", "fs")
VMEM_LIMIT = 56 * 1024 * 1024


def z_pairs(step):
    return [(z * 4 + y, ((z + step) % 16) * 4 + y) for z in range(16) for y in range(4)]


def y_pairs(mask):
    return [(z * 4 + y, z * 4 + (y ^ mask)) for z in range(16) for y in range(4)]


def z_send(value, step):
    return lax.ppermute(value, ZY, z_pairs(step))


def y_send(value, mask):
    return lax.ppermute(value, ZY, y_pairs(mask))


def core_swap(value):
    return lax.ppermute(value, "tp", [(t, t ^ 1) for t in range(8)])


X_GROUPS = [[0, 2, 4, 6], [1, 3, 5, 7]]


def x_exchange(pieces):
    return lax.all_to_all(pieces, "tp", 0, 0, axis_index_groups=X_GROUPS, tiled=True)


def z_gather(own, far_step):
    up, down = own, own
    got = {0: own}
    for k in range(1, 4):
        up = z_send(up, 1)
        down = z_send(down, -1)
        got[-k], got[k] = up, down
    got[4] = z_send(up, 1) if far_step > 0 else z_send(down, -1)
    return [got[d] for d in OFFSETS]


def y_gather(own, split):
    first = y_send(own, 1)
    third = y_send(own, 3)
    if split:
        cut = own.shape[0] // 2
        second = (y_send(first[:cut], 3), y_send(third[cut:], 1))
    else:
        second = (y_send(first, 3),)
    return own, first, second, third


def low_lanes(rows):
    return lax.broadcasted_iota(jnp.int32, (rows, 128), 1) < 64


def turn(tile):
    return pltpu.roll(tile, 64, 1)


def to_a(load, z, y, rows):
    odd = jnp.full((rows, 128), y & 1, jnp.int32) == 1
    tiles = []
    for d in OFFSETS:
        base = pl.multiple_of(((z + d) & 7) * 256, 256)
        for t in range(2):
            start = pl.multiple_of(base + 128 * ((y >> 1) ^ t), 128)
            tile = load(start)
            tiles.append(jnp.where(odd, turn(tile), tile))
    return tiles


def a_to_b(tiles, rows):
    low = low_lanes(rows)
    out = []
    for e in range(4):
        t, h = e >> 1, e & 1
        for j in range(4):
            first, second = tiles[4 * j + t], tiles[4 * j + 2 + t]
            if h == 0:
                out.append(jnp.where(low, first, turn(second)))
            else:
                out.append(jnp.where(low, turn(first), second))
    return out


def b_to_a(tiles, rows):
    low = low_lanes(rows)
    out = []
    for i in range(8):
        j = i // 2
        for t in range(2):
            even, odd = tiles[8 * t + j], tiles[8 * t + 4 + j]
            if i % 2 == 0:
                out.append(jnp.where(low, even, turn(odd)))
            else:
                out.append(jnp.where(low, turn(even), odd))
    return out


def norm_kernel(where_ref, x_ref, gain_ref, out_ref, keep_ref):
    z, y = where_ref[0], where_ref[1]
    gain = gain_ref[...]
    step = 48

    def rows_of(r, carry):
        start = pl.multiple_of(r * step, 16)
        x = x_ref[pl.ds(start, step), :].astype(F32)
        keep_ref[...] = x * lax.rsqrt(jnp.mean(x * x, axis=-1, keepdims=True) + EPS) * gain
        tiles = to_a(lambda s: keep_ref[:, pl.ds(s, 128)], z, y, step)
        for k, tile in enumerate(a_to_b(tiles, step)):
            out_ref[pl.ds(start, step), 128 * k : 128 * (k + 1)] = tile.astype(BF)
        return carry

    lax.fori_loop(0, ROWS // step, rows_of, 0)


def level_masks():
    t = np.arange(BLOCK)[:, None]
    u = np.arange(BLOCK)[None, :]
    rows, pairs = [], []
    for h in LEVELS:
        edge = (t // (2 * h)) * 2 * h + h
        later = t >= edge
        rows.append(np.where(later, (u >= edge) & (u <= t), (u > t) & (u < edge)))
        pairs.append(later & (u < edge) & (t // (2 * h) == u // (2 * h)))
    rows.append(u <= t)
    rows.append(u > t)
    return (
        np.concatenate(rows, 0).astype(np.float32),
        np.concatenate(pairs, 0).astype(np.float32),
    )


def silu(v):
    return v / (1.0 + jnp.exp(-v))


NT = (((1,), (1,)), ((), ()))
TN = (((0,), (0,)), ((), ()))


def mixing_kernel(
    where_ref,
    x_ref,
    w0_ref,
    w1_ref,
    w2a_ref,
    w2b_ref,
    w3_ref,
    scale_ref,
    shift_ref,
    burst_ref,
    gain_ref,
    spans_ref,
    pairs_ref,
    keep_ref,
    send_ref,
    q_ref,
    k_ref,
    v_ref,
    ld_ref,
    gate_ref,
    att_ref,
    state_ref,
):
    core = where_ref[2]
    parts = ((0, 512, w0_ref), (512, 512, w1_ref), (1024, 256, w2a_ref), (1280, 256, w2b_ref), (1536, 512, w3_ref))

    def project(lo, hi):
        total = None
        for start, size, ref in parts:
            piece = jnp.dot(
                x_ref[:, start : start + size], ref[:, lo:hi], preferred_element_type=F32
            )
            total = piece if total is None else total + piece
        return total * scale_ref[:, lo:hi]

    q_ref[...] = (silu(project(0, 128)) * 128**-0.5).astype(BF).astype(F32)
    k_ref[...] = silu(project(128, 256)).astype(BF).astype(F32)
    pre = project(256, 384) + shift_ref[...]
    soft = jnp.minimum(pre, 0.0) - jnp.log1p(jnp.exp(-jnp.abs(pre)))
    ld_ref[...] = soft * (1.0 / 16.0) + burst_ref[...]
    v_ref[...] = silu(project(384, 640)).astype(BF)
    gate_ref[...] = silu(project(640, 896))
    same = lax.broadcasted_iota(jnp.int32, (BLOCK, BLOCK), 0) == lax.broadcasted_iota(
        jnp.int32, (BLOCK, BLOCK), 1
    )
    state_ref[...] = jnp.zeros_like(state_ref)
    for b in range(ROWS // BLOCK):
        at = slice(b * BLOCK, (b + 1) * BLOCK)
        q, k, v = q_ref[at, :], k_ref[at, :], v_ref[at, :]
        reach = jnp.exp(
            jnp.dot(spans_ref[...], ld_ref[at, :], precision=HI, preferred_element_type=F32)
        )
        scores = jnp.where(same, jnp.sum(q * k, axis=-1, keepdims=True), 0.0)
        for n in range(len(LEVELS)):
            level = reach[n * BLOCK : (n + 1) * BLOCK, :]
            product = lax.dot_general(
                (q * level).astype(BF), (k * level).astype(BF), NT, preferred_element_type=F32
            )
            scores = scores + product * pairs_ref[n * BLOCK : (n + 1) * BLOCK, :]
        n = len(LEVELS)
        into = reach[n * BLOCK : (n + 1) * BLOCK, :]
        rest = reach[(n + 1) * BLOCK : (n + 2) * BLOCK, :]
        state = state_ref[...]
        o = jnp.dot(scores.astype(BF), v, preferred_element_type=F32) + lax.dot_general(
            (q * into).astype(BF), state.astype(BF), NT, preferred_element_type=F32
        )
        state_ref[...] = state * into[BLOCK - 1 :, :] + lax.dot_general(
            v, (k * rest).astype(BF), TN, preferred_element_type=F32
        )
        o = o * lax.rsqrt(jnp.mean(o * o, axis=-1, keepdims=True) + EPS)
        att_ref[at, :] = (o * gain_ref[...] * gate_ref[at, :]).astype(BF)
    half = ROWS // 2
    for ref, which in ((keep_ref, core), (send_ref, 1 - core)):
        rows = att_ref[pl.ds(pl.multiple_of(which * half, half), half), :]
        for start, size, w in parts:
            ref[:, start : start + size] = lax.dot_general(
                rows, w[:, 896:1152], NT, preferred_element_type=F32
            ).astype(BF)


def middle_kernel(where_ref, parts_ref, x_ref, gain_ref, residual_ref, normed_ref):
    z, y = where_ref[0], where_ref[1]
    rows = 48
    mixed = []
    for k in range(16):
        at = slice(128 * k, 128 * (k + 1))
        total = parts_ref[0, :, at].astype(F32)
        for s in range(1, 4):
            total = total + parts_ref[s, :, at].astype(F32)
        mixed.append(total)
    mixed = b_to_a(mixed, rows)
    own = to_a(lambda s: x_ref[:, pl.ds(s, 128)].astype(F32), z, y, rows)
    gain = to_a(lambda s: jnp.broadcast_to(gain_ref[:, pl.ds(s, 128)], (rows, 128)), z, y, rows)
    square = jnp.zeros((rows, 1), F32)
    kept = []
    for k in range(16):
        tile = (own[k] + mixed[k]).astype(BF)
        residual_ref[:, 128 * k : 128 * (k + 1)] = tile
        tile = tile.astype(F32)
        kept.append(tile)
        square = square + jnp.sum(tile * tile, axis=-1, keepdims=True)
    factor = lax.rsqrt(square * (1.0 / D) + EPS)
    for k in range(16):
        normed_ref[:, 128 * k : 128 * (k + 1)] = (kept[k] * factor * gain[k]).astype(BF)


def ffn_kernel(where_ref, own_ref, other_ref, scale_ref, *refs):
    blocks, (keep_ref, send_ref, hidden_ref) = refs[:8], refs[8:]
    for half, ref in ((0, own_ref), (1, other_ref)):
        for lo in range(0, 1024, 256):
            total = None
            for i in range(8):
                piece = jnp.dot(
                    ref[:, 256 * i : 256 * (i + 1)],
                    blocks[i][:, lo : lo + 256],
                    preferred_element_type=F32,
                )
                total = piece if total is None else total + piece
            value = jnp.maximum(total * scale_ref[:, lo : lo + 256], 0.0)
            hidden_ref[half, :, lo : lo + 256] = (value * value).astype(BF)
    for half, ref in ((0, keep_ref), (1, send_ref)):
        for i in range(8):
            ref[:, 256 * i : 256 * (i + 1)] = lax.dot_general(
                hidden_ref[half], blocks[i][:, 1024:2048], NT, preferred_element_type=F32
            ).astype(BF)


def last_kernel(where_ref, parts_ref, residual_ref, out_ref):
    z, y = where_ref[0], where_ref[1]
    rows = 48
    odd = jnp.full((rows, 128), y & 1, jnp.int32) == 1
    for i, d in enumerate(OFFSETS):
        base = pl.multiple_of(((z + d) & 7) * 256, 256)
        for t in range(2):
            at = slice(256 * i + 128 * t, 256 * i + 128 * (t + 1))
            total = parts_ref[0, :, at].astype(F32)
            for s in range(1, 4):
                total = total + parts_ref[s, :, at].astype(F32)
            tile = residual_ref[:, at].astype(F32) + total
            tile = jnp.where(odd, turn(tile), tile)
            start = pl.multiple_of(base + 128 * ((y >> 1) ^ t), 128)
            out_ref[:, pl.ds(start, 128)] = tile.astype(BF)


def place_kernel(where_ref, own_ref, other_ref, out_ref):
    core = where_ref[2]
    half = ROWS // 2
    out_ref[pl.ds(pl.multiple_of(core * half, half), half), :] = own_ref[...]
    out_ref[pl.ds(pl.multiple_of((1 - core) * half, half), half), :] = other_ref[...]


def call(kernel, name, outs, scratch, where, *args):
    vmem = pl.BlockSpec(memory_space=pltpu.VMEM)
    return pl.pallas_call(
        kernel,
        out_shape=[jax.ShapeDtypeStruct(s, t) for s, t in outs],
        in_specs=[pl.BlockSpec(memory_space=pltpu.SMEM)] + [vmem] * len(args),
        out_specs=[vmem] * len(outs),
        scratch_shapes=[pltpu.VMEM(s, t) for s, t in scratch],
        compiler_params=pltpu.CompilerParams(vmem_limit_bytes=VMEM_LIMIT),
        name=name,
    )(where, *args)


def body(
    x,
    pre_gain,
    w_probe,
    s_probe,
    w_lookup,
    s_lookup,
    w_forget,
    s_forget,
    shift,
    burst,
    w_content,
    s_content,
    w_filter,
    s_filter,
    head_gain,
    w_emission,
    s_emission,
    mlp_gain,
    w_raising,
    s_raising,
    w_lowering,
    s_lowering,
):
    fs = lax.axis_index("fs")
    tp = lax.axis_index("tp")
    where = jnp.stack([fs // 4, fs % 4, tp % 2, tp // 2]).astype(jnp.int32)
    attention = jnp.concatenate(
        [
            w_probe.astype(BF),
            w_lookup.astype(BF),
            w_forget.astype(BF),
            w_content.astype(BF),
            w_filter.astype(BF),
            (w_emission.T * s_emission[:, None]).astype(BF),
        ],
        axis=1,
    )
    ffn = jnp.concatenate(
        [w_raising.astype(BF), (w_lowering.T * s_lowering[:, None]).astype(BF)], axis=1
    )
    along_z = jnp.concatenate(z_gather(attention, 1), axis=0)
    w0, w1, (w2a, w2b), w3 = y_gather(along_z, True)
    f0, f1, (f2,), f3 = y_gather(ffn, False)
    blocks = z_gather(jnp.concatenate([f0, f1, f2, f3], axis=0), -1)

    (normed,) = call(
        norm_kernel, "norm", [((ROWS, D), BF)], [((48, D), F32)], where, x, pre_gain[None, :]
    )
    scales = jnp.concatenate([s_probe, s_lookup, s_forget, s_content, s_filter])[None, :]
    spans, pairs = level_masks()
    keep, send = call(
        mixing_kernel,
        "mixing",
        [((ROWS // 2, D), BF)] * 2,
        [
            ((ROWS, 128), F32),
            ((ROWS, 128), F32),
            ((ROWS, 256), BF),
            ((ROWS, 128), F32),
            ((ROWS, 256), F32),
            ((ROWS, 256), BF),
            ((256, 128), F32),
        ],
        where,
        normed,
        w0,
        w1,
        w2a,
        w2b,
        w3,
        scales,
        shift[None, :],
        burst,
        head_gain[None, :],
        jnp.asarray(spans),
        jnp.asarray(pairs),
    )

    def reduce_rows(keep, send):
        both = keep.astype(F32) + core_swap(send).astype(F32)
        return x_exchange(both.astype(BF).reshape(4, 48, D))

    def spread_rows(share):
        half = x_exchange(jnp.broadcast_to(share[None], (4, 48, D))).reshape(ROWS // 2, D)
        return half, core_swap(half)

    own_rows = lax.dynamic_slice_in_dim(x, where[2] * 192 + where[3] * 48, 48, 0)
    residual, normed_share = call(
        middle_kernel,
        "middle",
        [((48, D), BF)] * 2,
        [],
        where,
        reduce_rows(keep, send),
        own_rows,
        mlp_gain[None, :],
    )
    own, other = spread_rows(normed_share)
    keep, send = call(
        ffn_kernel,
        "ffn",
        [((ROWS // 2, D), BF)] * 2,
        [((2, ROWS // 2, 1024), BF)],
        where,
        own,
        other,
        s_raising[None, :],
        *blocks,
    )
    (share,) = call(
        last_kernel, "last", [((48, D), BF)], [], where, reduce_rows(keep, send), residual
    )
    own, other = spread_rows(share)
    (out,) = call(place_kernel, "place", [((ROWS, D), BF)], [], where, own, other)
    return out


def solution(mesh):
    return jax.shard_map(
        body,
        mesh=mesh,
        in_specs=(
            P(("rep", "fs"), None),
            P(),
            P("fs", "tp"),
            P("tp"),
            P("fs", "tp"),
            P("tp"),
            P("fs", "tp"),
            P("tp"),
            P("tp"),
            P(("rep", "fs"), "tp"),
            P("fs", "tp"),
            P("tp"),
            P("fs", "tp"),
            P("tp"),
            P("tp"),
            P("tp", "fs"),
            P("fs"),
            P(),
            P("fs", "tp"),
            P("tp"),
            P("tp", "fs"),
            P("fs"),
        ),
        out_specs=P(("rep", "fs"), None),
        check_vma=False,
    )
```

```python
import jax
import jax.numpy as jnp
from jax import lax
from jax.experimental import pallas as pl
from jax.experimental.pallas import tpu as pltpu
from jax.sharding import PartitionSpec as P


EPS = 1e-06
BLOCK = 64
ROWS = 384
D = 2048
BF = jnp.bfloat16
F32 = jnp.float32
HI = lax.Precision.HIGHEST
OFFSETS = (0, -1, 1, -2, 2, -3, 3, 4)
LEVELS = (32, 16, 8, 4, 2, 1)
ZY = ("rep", "fs")
EXTRA = 512
VMEM_LIMIT = 10 * 1024 * 1024


def z_pairs(step):
    return [(z * 4 + y, ((z + step) % 16) * 4 + y) for z in range(16) for y in range(4)]


def y_pairs(mask):
    return [(z * 4 + y, z * 4 + (y ^ mask)) for z in range(16) for y in range(4)]


def z_send(value, step):
    return lax.ppermute(value, ZY, z_pairs(step))


def y_send(value, mask):
    return lax.ppermute(value, ZY, y_pairs(mask))


def x_send(value, mask):
    return lax.ppermute(value, "tp", [(t, t ^ (2 * mask)) for t in range(8)])


def core_swap(value):
    return lax.ppermute(value, "tp", [(t, t ^ 1) for t in range(8)])


def z_gather(own, far_step):
    up, down = own, own
    got = {0: own}
    for k in range(1, 4):
        up = z_send(up, 1)
        down = z_send(down, -1)
        got[-k], got[k] = up, down
    got[4] = z_send(up if far_step > 0 else down, far_step)
    return [got[d] for d in OFFSETS]


def y_gather(own):
    first = y_send(own, 1)
    third = y_send(own, 3)
    cut = own.shape[0] // 2
    return (own, first, y_send(first[:cut], 3), y_send(third[cut:], 1), third)


def y_direct(own):
    far = y_send(own, 2)
    return own, y_send(own, 1), far, y_send(own, 3)


def low_lanes(rows):
    return lax.broadcasted_iota(jnp.int32, (rows, 128), 1) < 64


def turn(tile):
    return pltpu.roll(tile, 64, 1)


def to_a(load, z):
    tiles = []
    for d in OFFSETS:
        base = pl.multiple_of(((z + d) & 7) * 256, 256)
        for t in range(2):
            tiles.append(load(pl.multiple_of(base + 128 * t, 128)))
    return tiles


def b_to_a(tiles, rows):
    low = low_lanes(rows)
    out = []
    for i in range(8):
        j = i // 2
        for t in range(2):
            even, odd = tiles[8 * t + j], tiles[8 * t + 4 + j]
            if i % 2 == 0:
                out.append(jnp.where(low, even, turn(odd)))
            else:
                out.append(jnp.where(low, turn(even), odd))
    return out


def a_to_b(tiles, rows):
    low = low_lanes(rows)
    out = []
    for y in range(4):
        t, h = y >> 1, y & 1
        for j in range(4):
            first, second = tiles[4 * j + t], tiles[4 * j + 2 + t]
            if h == 0:
                out.append(jnp.where(low, first, turn(second)))
            else:
                out.append(jnp.where(low, turn(first), second))
    return out


def cast_kernel(*refs):
    sources, (attention, ffn), held, sems = refs[:10], refs[10:12], refs[12:22], refs[22]
    copies = [pltpu.make_async_copy(s, h, sems.at[n]) for n, (s, h) in enumerate(zip(sources, held))]
    for copy in copies:
        copy.start()
    eye = lax.broadcasted_iota(jnp.int32, (64, 64), 0) == lax.broadcasted_iota(
        jnp.int32, (64, 64), 1
    )

    def column(ref):
        return jnp.sum(jnp.where(eye, ref[...], 0.0), axis=-1, keepdims=True)

    at = 0
    for n in range(5):
        copies[n].wait()
        attention[:, at : at + held[n].shape[1]] = held[n][...].astype(BF)
        at += held[n].shape[1]
    copies[5].wait()
    copies[8].wait()
    attention[:, at:1152] = (held[5][...] * column(held[8])).astype(BF)
    copies[7].wait()
    copies[9].wait()
    low = (held[7][...] * column(held[9])).astype(BF)
    attention[:, 1152:] = low[:, :EXTRA]
    ffn[:, 1024:] = low[:, EXTRA:]
    copies[6].wait()
    ffn[:, :1024] = held[6][...].astype(BF)


def stack_kernel(*refs):
    blocks, (tables_ref, low_ref) = refs[:8], refs[8:]
    for n, ref in enumerate(blocks):
        at = slice(64 * n, 64 * (n + 1))
        tables_ref[at, :] = ref[:, :1152]
        low_ref[at, :] = ref[:, 1152:]


def rows_kernel(where_ref, *refs):
    blocks, out_ref = refs[:4], refs[4]
    for mask, ref in enumerate(blocks):
        out_ref[pl.ds(pl.multiple_of((where_ref[1] ^ mask) * 64, 64), 64), :] = ref[...]


def half_kernel(where_ref, *refs):
    blocks, out_ref = refs[:4], refs[4]
    for mask, ref in enumerate(blocks):
        out_ref[pl.ds(pl.multiple_of((where_ref[3] ^ mask) * 48, 48), 48), :] = ref[...]


def join_kernel(where_ref, keep_ref, got_ref, *outs):
    for mask, ref in enumerate(outs):
        at = pl.ds(pl.multiple_of((where_ref[3] ^ mask) * 48, 48), 48)
        ref[...] = (keep_ref[at, :].astype(F32) + got_ref[at, :].astype(F32)).astype(BF)


def norm_kernel(where_ref, x_ref, gain_ref, out_ref, keep_ref):
    z, y = where_ref[0], where_ref[1]
    gain = gain_ref[...]
    step = 48

    def rows_of(r, carry):
        start = pl.multiple_of(r * step, 16)
        x = x_ref[pl.ds(start, step), :].astype(F32)
        keep_ref[...] = x * lax.rsqrt(jnp.mean(x * x, axis=-1, keepdims=True) + EPS) * gain
        tiles = a_to_b(to_a(lambda s: keep_ref[:, pl.ds(s, 128)], z), step)
        for k, tile in enumerate(tiles):
            place = pl.multiple_of((y ^ (k // 4)) * 512 + 128 * (k % 4), 128)
            out_ref[pl.ds(start, step), pl.ds(place, 128)] = tile.astype(BF)
        return carry

    lax.fori_loop(0, ROWS // step, rows_of, 0)


def spans_and_pairs():
    t = lax.broadcasted_iota(jnp.int32, (BLOCK, BLOCK), 0)
    u = lax.broadcasted_iota(jnp.int32, (BLOCK, BLOCK), 1)
    spans, pairs = [], []
    for h in LEVELS:
        group = (t | (2 * h - 1)) ^ (2 * h - 1)
        edge = group + h
        later = (t & h) != 0
        ahead = (u >= edge) & (u <= t)
        behind = (u > t) & (u < edge)
        spans.append((later & ahead) | (~later & behind))
        pairs.append(later & (u >= group) & (u < edge))
    spans += [u <= t, u > t]
    return jnp.concatenate([jnp.where(m, 1.0, 0.0) for m in spans], axis=0), pairs, u == t


def silu(v):
    return v / (1.0 + jnp.exp(-v))


NT = (((1,), (1,)), ((), ()))
TN = (((0,), (0,)), ((), ()))


def mixing_kernel(
    where_ref,
    x_ref,
    w0_ref,
    w1_ref,
    w2a_ref,
    w2b_ref,
    w3_ref,
    probe_scale,
    lookup_scale,
    forget_scale,
    content_scale,
    gate_scale,
    shift_ref,
    burst_ref,
    gain_ref,
    keep_ref,
    send_ref,
    q_ref,
    k_ref,
    v_ref,
    ld_ref,
    gate_ref,
    att_ref,
    state_ref,
):
    core = where_ref[2]
    parts = (
        (0, 0, 512, w0_ref),
        (1, 0, 512, w1_ref),
        (2, 0, 256, w2a_ref),
        (2, 256, 256, w2b_ref),
        (3, 0, 512, w3_ref),
    )

    def project(lo, hi, scale):
        total = None
        for mask, start, size, ref in parts:
            at = 512 * mask + start
            piece = jnp.dot(
                x_ref[:, at : at + size], ref[:, lo:hi], preferred_element_type=F32
            )
            total = piece if total is None else total + piece
        return total * scale[...]

    q_ref[...] = (silu(project(0, 128, probe_scale)) * 128**-0.5).astype(BF).astype(F32)
    k_ref[...] = silu(project(128, 256, lookup_scale)).astype(BF).astype(F32)
    pre = project(256, 384, forget_scale) + shift_ref[...]
    soft = jnp.minimum(pre, 0.0) - jnp.log1p(jnp.exp(-jnp.abs(pre)))
    eye = lax.broadcasted_iota(jnp.int32, (128, 128), 0) == lax.broadcasted_iota(
        jnp.int32, (128, 128), 1
    )
    for b in range(3):
        at = slice(128 * b, 128 * (b + 1))
        burst = jnp.sum(jnp.where(eye, burst_ref[:, at], 0.0), axis=-1, keepdims=True)
        ld_ref[at, :] = soft[at, :] * (1.0 / 16.0) + burst
    v_ref[...] = silu(project(384, 640, content_scale)).astype(BF)
    gate_ref[...] = silu(project(640, 896, gate_scale))
    spans, pairs, same = spans_and_pairs()
    state_ref[...] = jnp.zeros_like(state_ref)
    for b in range(ROWS // BLOCK):
        at = slice(b * BLOCK, (b + 1) * BLOCK)
        q, k, v = q_ref[at, :], k_ref[at, :], v_ref[at, :]
        reach = jnp.exp(
            jnp.dot(spans, ld_ref[at, :], precision=HI, preferred_element_type=F32)
        )
        scores = jnp.where(same, jnp.sum(q * k, axis=-1, keepdims=True), 0.0)
        for n in range(len(LEVELS)):
            level = reach[n * BLOCK : (n + 1) * BLOCK, :]
            product = lax.dot_general(
                (q * level).astype(BF), (k * level).astype(BF), NT, preferred_element_type=F32
            )
            scores = jnp.where(pairs[n], product, scores)
        n = len(LEVELS)
        into = reach[n * BLOCK : (n + 1) * BLOCK, :]
        rest = reach[(n + 1) * BLOCK : (n + 2) * BLOCK, :]
        state = state_ref[...]
        o = jnp.dot(scores.astype(BF), v, preferred_element_type=F32) + lax.dot_general(
            (q * into).astype(BF), state.astype(BF), NT, preferred_element_type=F32
        )
        state_ref[...] = state * into[BLOCK - 1 :, :] + lax.dot_general(
            v, (k * rest).astype(BF), TN, preferred_element_type=F32
        )
        o = o * lax.rsqrt(jnp.mean(o * o, axis=-1, keepdims=True) + EPS)
        att_ref[at, :] = (o * gain_ref[...] * gate_ref[at, :]).astype(BF)
    half = ROWS // 2
    for ref, which in ((keep_ref, core), (send_ref, 1 - core)):
        rows = att_ref[pl.ds(pl.multiple_of(which * half, half), half), :]
        for mask, start, size, w in parts:
            at = pl.multiple_of((where_ref[1] ^ mask) * 512 + start, 256)
            ref[:, pl.ds(at, size)] = lax.dot_general(
                rows, w[:, 896:1152], NT, preferred_element_type=F32
            ).astype(BF)


def middle_kernel(where_ref, x_ref, gain_ref, *refs):
    parts, (residual_ref, normed_ref) = refs[:4], refs[4:]
    z = where_ref[0]
    rows = 48
    mixed = []
    for k in range(16):
        at = slice(128 * k, 128 * (k + 1))
        total = parts[0][:, at].astype(F32)
        for part in parts[1:]:
            total = total + part[:, at].astype(F32)
        mixed.append(total)
    mixed = b_to_a(mixed, rows)
    own = to_a(lambda s: x_ref[:, pl.ds(s, 128)].astype(F32), z)
    gain = to_a(lambda s: gain_ref[:, pl.ds(s, 128)], z)
    square = jnp.zeros((rows, 1), F32)
    kept = []
    for k in range(16):
        tile = (own[k] + mixed[k]).astype(BF)
        residual_ref[:, 128 * k : 128 * (k + 1)] = tile
        tile = tile.astype(F32)
        kept.append(tile)
        square = square + jnp.sum(tile * tile, axis=-1, keepdims=True)
    factor = lax.rsqrt(square * (1.0 / D) + EPS)
    for k in range(16):
        normed_ref[:, 128 * k : 128 * (k + 1)] = (kept[k] * factor * gain[k]).astype(BF)


def ffn_kernel(where_ref, own_ref, other_ref, scale_ref, *refs):
    lows, refs = refs[:4], refs[4:]
    pieces, (keep_ref, send_ref, hidden_ref, part_ref) = refs[:8], refs[8:]
    for half, ref in ((0, own_ref), (1, other_ref)):
        for lo in range(0, 1024, 256):
            total = None
            for i, piece in enumerate(pieces):
                part = jnp.dot(
                    ref[:, 256 * i : 256 * (i + 1)],
                    piece[:, lo : lo + 256],
                    preferred_element_type=F32,
                )
                total = part if total is None else total + part
            value = jnp.maximum(total * scale_ref[:, lo : lo + 256], 0.0)
            hidden_ref[half, :, lo : lo + 256] = (value * value).astype(BF)
    rows = ROWS // 2
    low = low_lanes(rows)
    for half, ref in ((1, send_ref), (0, keep_ref)):
        for y in range(4):
            part_ref[where_ref[1] ^ y] = lax.dot_general(
                hidden_ref[half, :, :EXTRA], lows[y][...], NT, preferred_element_type=F32
            )
        for i, piece in enumerate(pieces):
            total = lax.dot_general(
                hidden_ref[half, :, EXTRA:], piece[:, 1024:], NT, preferred_element_type=F32
            )
            at = slice(128 * (i // 2), 128 * (i // 2 + 1))
            for t in range(2):
                even, odd = part_ref[2 * t, :, at], part_ref[2 * t + 1, :, at]
                if i % 2 == 0:
                    extra = jnp.where(low, even, turn(odd))
                else:
                    extra = jnp.where(low, turn(even), odd)
                ref[:, 256 * i + 128 * t : 256 * i + 128 * (t + 1)] = (
                    total[:, 128 * t : 128 * (t + 1)] + extra
                ).astype(BF)


def last_kernel(where_ref, residual_ref, *refs):
    parts, out_ref = refs[:4], refs[4]
    for i, d in enumerate(OFFSETS):
        base = pl.multiple_of(((where_ref[0] + d) & 7) * 256, 256)
        at = slice(256 * i, 256 * (i + 1))
        total = parts[0][:, at].astype(F32)
        for part in parts[1:]:
            total = total + part[:, at].astype(F32)
        out_ref[:, pl.ds(base, 256)] = (residual_ref[:, at].astype(F32) + total).astype(BF)


def place_own_kernel(where_ref, own_ref, out_ref, sem):
    half = ROWS // 2
    start = pl.multiple_of(where_ref[2] * half, half)
    copy = pltpu.make_async_copy(own_ref, out_ref.at[pl.ds(start, half), :], sem)
    copy.start()
    copy.wait()


def place_other_kernel(where_ref, other_ref, held_ref, out_ref, sem):
    half = ROWS // 2
    start = pl.multiple_of((1 - where_ref[2]) * half, half)
    copy = pltpu.make_async_copy(other_ref, out_ref.at[pl.ds(start, half), :], sem)
    copy.start()
    copy.wait()


def near(value):
    return pltpu.with_memory_space_constraint(value, pltpu.VMEM)


def call(kernel, outs, scratch, *args):
    vmem = pl.BlockSpec(memory_space=pltpu.VMEM)
    smem = pl.BlockSpec(memory_space=pltpu.SMEM)
    return pl.pallas_call(
        kernel,
        out_shape=[pltpu.VMEM(s, t) for s, t in outs],
        in_specs=[smem if a.dtype == jnp.int32 else vmem for a in args],
        out_specs=[vmem] * len(outs),
        scratch_shapes=[pltpu.VMEM(s, t) for s, t in scratch],
        compiler_params=pltpu.CompilerParams(vmem_limit_bytes=VMEM_LIMIT),
    )(*args)


def place(where, own, other):
    vmem = pl.BlockSpec(memory_space=pltpu.VMEM)
    smem = pl.BlockSpec(memory_space=pltpu.SMEM)
    far = pl.BlockSpec(memory_space=pl.ANY)
    shape = jax.ShapeDtypeStruct((ROWS, D), BF)
    held = pl.pallas_call(
        place_own_kernel,
        out_shape=shape,
        in_specs=[smem, vmem],
        out_specs=far,
        scratch_shapes=[pltpu.SemaphoreType.DMA],
        compiler_params=pltpu.CompilerParams(vmem_limit_bytes=VMEM_LIMIT),
        name="place_own",
    )(where, near(own))
    return pl.pallas_call(
        place_other_kernel,
        out_shape=shape,
        in_specs=[smem, vmem, far],
        out_specs=far,
        scratch_shapes=[pltpu.SemaphoreType.DMA],
        input_output_aliases={2: 0},
        compiler_params=pltpu.CompilerParams(vmem_limit_bytes=VMEM_LIMIT),
        name="place_other",
    )(where, near(other), held)


def body(
    x,
    pre_gain,
    w_probe,
    s_probe,
    w_lookup,
    s_lookup,
    w_forget,
    s_forget,
    shift,
    burst,
    w_content,
    s_content,
    w_filter,
    s_filter,
    head_gain,
    w_emission,
    s_emission,
    mlp_gain,
    w_raising,
    s_raising,
    w_lowering,
    s_lowering,
):
    fs = lax.axis_index("fs")
    tp = lax.axis_index("tp")
    where = jnp.stack([fs >> 2, fs & 3, tp & 1, tp >> 1]).astype(jnp.int32)
    tables = (
        w_probe,
        w_lookup,
        w_forget,
        w_content,
        w_filter,
        w_emission.T,
        w_raising,
        w_lowering.T,
        s_emission[None, :],
        s_lowering[None, :],
    )
    vmem = pl.BlockSpec(memory_space=pltpu.VMEM)
    far = pl.BlockSpec(memory_space=pl.ANY)
    attention, ffn = pl.pallas_call(
        cast_kernel,
        out_shape=[pltpu.VMEM((64, 1152 + EXTRA), BF), pltpu.VMEM((64, 2048 - EXTRA), BF)],
        in_specs=[far] * 10,
        out_specs=[vmem] * 2,
        scratch_shapes=[pltpu.VMEM(w.shape, F32) for w in tables]
        + [pltpu.SemaphoreType.DMA((10,))],
        compiler_params=pltpu.CompilerParams(vmem_limit_bytes=VMEM_LIMIT),
        name="cast",
    )(
        *(pltpu.with_memory_space_constraint(w, pltpu.HBM) for w in tables)
    )
    along_z, low_z = call(
        stack_kernel,
        [((512, 1152), BF), ((512, EXTRA), BF)],
        [],
        *(near(b) for b in z_gather(attention, 1)),
    )
    tables = y_gather(along_z)
    extra = y_direct(low_z)
    (along_y,) = call(
        rows_kernel, [((256, 2048 - EXTRA), BF)], [], where, *(near(b) for b in y_direct(ffn))
    )
    pieces = z_gather(along_y, 1)

    (normed,) = call(norm_kernel, [((ROWS, D), BF)], [((48, D), F32)], where, x, pre_gain[None, :])
    keep, send = call(
        mixing_kernel,
        [((ROWS // 2, D), BF)] * 2,
        [
            ((ROWS, 128), F32),
            ((ROWS, 128), F32),
            ((ROWS, 256), BF),
            ((ROWS, 128), F32),
            ((ROWS, 256), F32),
            ((ROWS, 256), BF),
            ((256, 128), F32),
        ],
        where,
        near(normed),
        *(near(t) for t in tables),
        s_probe[None, :],
        s_lookup[None, :],
        s_forget[None, :],
        s_content[None, :],
        s_filter[None, :],
        shift[None, :],
        burst.T,
        head_gain[None, :],
    )

    piece = ((48, D), BF)

    def reduce_rows(keep, send):
        own, *others = call(join_kernel, [piece] * 4, [], where, near(keep), near(core_swap(send)))
        got = {m: x_send(others[m - 1], m) for m in (2, 1, 3)}
        return near(own), near(got[1]), near(got[2]), near(got[3])

    def spread_rows(own):
        got = {m: x_send(own, m) for m in (2, 1, 3)}
        (half,) = call(
            half_kernel,
            [((ROWS // 2, D), BF)],
            [],
            where,
            near(own),
            near(got[1]),
            near(got[2]),
            near(got[3]),
        )
        return half, core_swap(half)

    own_rows = lax.dynamic_slice_in_dim(x, where[2] * 192 + where[3] * 48, 48, 0)
    residual, normed_share = call(
        middle_kernel, [piece] * 2, [], where, own_rows, mlp_gain[None, :], *reduce_rows(keep, send)
    )
    own, other = spread_rows(normed_share)
    keep, send = call(
        ffn_kernel,
        [((ROWS // 2, D), BF)] * 2,
        [((2, ROWS // 2, 1024), BF), ((4, ROWS // 2, 512), F32)],
        where,
        near(own),
        near(other),
        s_raising[None, :],
        *(near(e) for e in extra),
        *(near(p) for p in pieces),
    )
    (share,) = call(last_kernel, [piece], [], where, near(residual), *reduce_rows(keep, send))
    return place(where, *spread_rows(share))


def solution(mesh):
    return jax.shard_map(
        body,
        mesh=mesh,
        in_specs=(
            P(("rep", "fs"), None),
            P(),
            P("fs", "tp"),
            P("tp"),
            P("fs", "tp"),
            P("tp"),
            P("fs", "tp"),
            P("tp"),
            P("tp"),
            P(("rep", "fs"), "tp"),
            P("fs", "tp"),
            P("tp"),
            P("fs", "tp"),
            P("tp"),
            P("tp"),
            P("tp", "fs"),
            P("fs"),
            P(),
            P("fs", "tp"),
            P("tp"),
            P("tp", "fs"),
            P("fs"),
        ),
        out_specs=P(("rep", "fs"), None),
        check_vma=False,
    )
```

```python
import jax
import jax.numpy as jnp
from jax import lax
from jax.experimental import pallas as pl
from jax.experimental.pallas import tpu as pltpu
from jax.sharding import PartitionSpec as P


EPS = 1e-06
BLOCK = 64
ROWS = 384
D = 2048
BF = jnp.bfloat16
F32 = jnp.float32
HI = lax.Precision.HIGHEST
OFFSETS = (0, -1, 1, -2, 2, -3, 3, 4)
LEVELS = (32, 16, 8, 4, 2, 1)
ZY = ("rep", "fs")
VMEM_LIMIT = 12 * 1024 * 1024


def z_pairs(step):
    return [(z * 4 + y, ((z + step) % 16) * 4 + y) for z in range(16) for y in range(4)]


def y_pairs(mask):
    return [(z * 4 + y, z * 4 + (y ^ mask)) for z in range(16) for y in range(4)]


def z_send(value, step):
    return lax.ppermute(value, ZY, z_pairs(step))


def y_send(value, mask):
    return lax.ppermute(value, ZY, y_pairs(mask))


def core_swap(value):
    return lax.ppermute(value, "tp", [(t, t ^ 1) for t in range(8)])


X_GROUPS = [[0, 2, 4, 6], [1, 3, 5, 7]]


def x_exchange(pieces):
    return lax.all_to_all(pieces, "tp", 0, 0, axis_index_groups=X_GROUPS, tiled=True)


def z_mixed(own):
    got = {0: own}
    for k in (1, 2):
        got[-k] = z_send(own, k)
        got[k] = z_send(own, -k)
    got[-3] = z_send(got[-2], 1)
    got[3] = z_send(got[2], -1)
    got[4] = z_send(got[-2], 2)
    return [got[d] for d in OFFSETS]


def z_relay(own):
    up, down = own, own
    got = {0: own}
    for k in range(1, 4):
        up = z_send(up, 1)
        down = z_send(down, -1)
        got[-k], got[k] = up, down
    got[4] = z_send(up, 1)
    return [got[d] for d in OFFSETS]


def y_gather(own):
    first = y_send(own, 1)
    third = y_send(own, 3)
    cut = own.shape[0] // 2
    return (
        (own, first, third),
        (y_send(first[:cut], 3), y_send(third[cut:], 1)),
    )


Y_GROUPS = [[4 * z + y for y in range(4)] for z in range(8)]


def y_exchange(pieces):
    return lax.all_to_all(pieces, "fs", 0, 0, axis_index_groups=Y_GROUPS, tiled=True)


def low_lanes(rows):
    return lax.broadcasted_iota(jnp.int32, (rows, 128), 1) < 64


def turn(tile):
    return pltpu.roll(tile, 64, 1)


def to_a(load, z):
    tiles = []
    for d in OFFSETS:
        base = pl.multiple_of(((z + d) & 7) * 256, 256)
        for t in range(2):
            tiles.append(load(pl.multiple_of(base + 128 * t, 128)))
    return tiles


def b_to_a(tiles, rows):
    low = low_lanes(rows)
    out = []
    for i in range(8):
        j = i // 2
        for t in range(2):
            even, odd = tiles[8 * t + j], tiles[8 * t + 4 + j]
            if i % 2 == 0:
                out.append(jnp.where(low, even, turn(odd)))
            else:
                out.append(jnp.where(low, turn(even), odd))
    return out


def a_to_b(tiles, rows):
    low = low_lanes(rows)
    out = []
    for y in range(4):
        t, h = y >> 1, y & 1
        for j in range(4):
            first, second = tiles[4 * j + t], tiles[4 * j + 2 + t]
            if h == 0:
                out.append(jnp.where(low, first, turn(second)))
            else:
                out.append(jnp.where(low, turn(first), second))
    return out


def cast_kernel(*refs):
    sources, (attention, ffn), held, sems = refs[:10], refs[10:12], refs[12:22], refs[22]
    copies = [pltpu.make_async_copy(s, h, sems.at[n]) for n, (s, h) in enumerate(zip(sources, held))]
    for copy in copies:
        copy.start()
    eye = lax.broadcasted_iota(jnp.int32, (64, 64), 0) == lax.broadcasted_iota(
        jnp.int32, (64, 64), 1
    )

    def column(ref):
        return jnp.sum(jnp.where(eye, ref[...], 0.0), axis=-1, keepdims=True)

    at = 0
    for n in range(5):
        copies[n].wait()
        attention[:, at : at + held[n].shape[1]] = held[n][...].astype(BF)
        at += held[n].shape[1]
    copies[5].wait()
    copies[8].wait()
    attention[:, at:] = (held[5][...] * column(held[8])).astype(BF)
    copies[7].wait()
    copies[9].wait()
    low = (held[7][...] * column(held[9])).astype(BF)
    copies[6].wait()
    up = held[6][...].astype(BF)
    for s in range(4):
        ffn[s, :, :1024] = up
        ffn[s, :, 1024:] = low


def stack_kernel(*refs):
    for n, ref in enumerate(refs[:-1]):
        refs[-1][64 * n : 64 * (n + 1), :] = ref[...]


def norm_kernel(where_ref, x_ref, gain_ref, out_ref, keep_ref):
    z, y = where_ref[0], where_ref[1]
    gain = gain_ref[...]
    step = 48

    def rows_of(r, carry):
        start = pl.multiple_of(r * step, 16)
        x = x_ref[pl.ds(start, step), :].astype(F32)
        keep_ref[...] = x * lax.rsqrt(jnp.mean(x * x, axis=-1, keepdims=True) + EPS) * gain
        tiles = a_to_b(to_a(lambda s: keep_ref[:, pl.ds(s, 128)], z), step)
        for k, tile in enumerate(tiles):
            place = pl.multiple_of((y ^ (k // 4)) * 512 + 128 * (k % 4), 128)
            out_ref[pl.ds(start, step), pl.ds(place, 128)] = tile.astype(BF)
        return carry

    lax.fori_loop(0, ROWS // step, rows_of, 0)


def spans_and_pairs():
    t = lax.broadcasted_iota(jnp.int32, (BLOCK, BLOCK), 0)
    u = lax.broadcasted_iota(jnp.int32, (BLOCK, BLOCK), 1)
    spans, pairs = [], []
    for h in LEVELS:
        group = (t | (2 * h - 1)) ^ (2 * h - 1)
        edge = group + h
        later = (t & h) != 0
        ahead = (u >= edge) & (u <= t)
        behind = (u > t) & (u < edge)
        spans.append((later & ahead) | (~later & behind))
        pairs.append(later & (u >= group) & (u < edge))
    spans += [u <= t, u > t]
    return jnp.concatenate([jnp.where(m, 1.0, 0.0) for m in spans], axis=0), pairs, u == t


def silu(v):
    return v / (1.0 + jnp.exp(-v))


NT = (((1,), (1,)), ((), ()))
TN = (((0,), (0,)), ((), ()))


def early_kernel(x_ref, w0_ref, w1_ref, w3_ref, out_ref):
    for lo in range(0, 896, 128):
        total = None
        for mask, ref in ((0, w0_ref), (1, w1_ref), (3, w3_ref)):
            piece = jnp.dot(
                x_ref[:, 512 * mask : 512 * (mask + 1)],
                ref[:, lo : lo + 128],
                preferred_element_type=F32,
            )
            total = piece if total is None else total + piece
        out_ref[:, lo : lo + 128] = total


def mixing_kernel(
    where_ref,
    x_ref,
    early_ref,
    w0_ref,
    w1_ref,
    w3_ref,
    w2a_ref,
    w2b_ref,
    probe_scale,
    lookup_scale,
    forget_scale,
    content_scale,
    gate_scale,
    shift_ref,
    burst_ref,
    gain_ref,
    keep_ref,
    send_ref,
    q_ref,
    k_ref,
    v_ref,
    ld_ref,
    gate_ref,
    att_ref,
    state_ref,
):
    core = where_ref[2]
    parts = (
        (0, 0, 512, w0_ref),
        (1, 0, 512, w1_ref),
        (2, 0, 256, w2a_ref),
        (2, 256, 256, w2b_ref),
        (3, 0, 512, w3_ref),
    )

    def project(lo, hi, scale):
        total = early_ref[:, lo:hi]
        for start, ref in ((1024, w2a_ref), (1280, w2b_ref)):
            total = total + jnp.dot(
                x_ref[:, start : start + 256], ref[:, lo:hi], preferred_element_type=F32
            )
        return total * scale[...]

    q_ref[...] = (silu(project(0, 128, probe_scale)) * 128**-0.5).astype(BF).astype(F32)
    k_ref[...] = silu(project(128, 256, lookup_scale)).astype(BF).astype(F32)
    pre = project(256, 384, forget_scale) + shift_ref[...]
    soft = jnp.minimum(pre, 0.0) - jnp.log1p(jnp.exp(-jnp.abs(pre)))
    eye = lax.broadcasted_iota(jnp.int32, (128, 128), 0) == lax.broadcasted_iota(
        jnp.int32, (128, 128), 1
    )
    for b in range(3):
        at = slice(128 * b, 128 * (b + 1))
        burst = jnp.sum(jnp.where(eye, burst_ref[:, at], 0.0), axis=-1, keepdims=True)
        ld_ref[at, :] = soft[at, :] * (1.0 / 16.0) + burst
    v_ref[...] = silu(project(384, 640, content_scale)).astype(BF)
    gate_ref[...] = silu(project(640, 896, gate_scale))
    spans, pairs, same = spans_and_pairs()
    state_ref[...] = jnp.zeros_like(state_ref)
    for b in range(ROWS // BLOCK):
        at = slice(b * BLOCK, (b + 1) * BLOCK)
        q, k, v = q_ref[at, :], k_ref[at, :], v_ref[at, :]
        reach = jnp.exp(
            jnp.dot(spans, ld_ref[at, :], precision=HI, preferred_element_type=F32)
        )
        scores = jnp.where(same, jnp.sum(q * k, axis=-1, keepdims=True), 0.0)
        for n in range(len(LEVELS)):
            level = reach[n * BLOCK : (n + 1) * BLOCK, :]
            product = lax.dot_general(
                (q * level).astype(BF), (k * level).astype(BF), NT, preferred_element_type=F32
            )
            scores = jnp.where(pairs[n], product, scores)
        n = len(LEVELS)
        into = reach[n * BLOCK : (n + 1) * BLOCK, :]
        rest = reach[(n + 1) * BLOCK : (n + 2) * BLOCK, :]
        state = state_ref[...]
        o = jnp.dot(scores.astype(BF), v, preferred_element_type=F32) + lax.dot_general(
            (q * into).astype(BF), state.astype(BF), NT, preferred_element_type=F32
        )
        state_ref[...] = state * into[BLOCK - 1 :, :] + lax.dot_general(
            v, (k * rest).astype(BF), TN, preferred_element_type=F32
        )
        o = o * lax.rsqrt(jnp.mean(o * o, axis=-1, keepdims=True) + EPS)
        att_ref[at, :] = (o * gain_ref[...] * gate_ref[at, :]).astype(BF)
    half = ROWS // 2
    for ref, which in ((keep_ref, core), (send_ref, 1 - core)):
        rows = att_ref[pl.ds(pl.multiple_of(which * half, half), half), :]
        for mask, start, size, w in parts:
            at = pl.multiple_of((where_ref[1] ^ mask) * 512 + start, 256)
            ref[:, pl.ds(at, size)] = lax.dot_general(
                rows, w[:, 896:1152], NT, preferred_element_type=F32
            ).astype(BF)


def middle_kernel(where_ref, parts_ref, x_ref, gain_ref, residual_ref, normed_ref):
    z = where_ref[0]
    rows = 48
    mixed = []
    for k in range(16):
        at = slice(128 * k, 128 * (k + 1))
        total = parts_ref[0, :, at].astype(F32)
        for s in range(1, 4):
            total = total + parts_ref[s, :, at].astype(F32)
        mixed.append(total)
    mixed = b_to_a(mixed, rows)
    own = to_a(lambda s: x_ref[:, pl.ds(s, 128)].astype(F32), z)
    gain = to_a(lambda s: gain_ref[:, pl.ds(s, 128)], z)
    square = jnp.zeros((rows, 1), F32)
    kept = []
    for k in range(16):
        tile = (own[k] + mixed[k]).astype(BF)
        residual_ref[:, 128 * k : 128 * (k + 1)] = tile
        tile = tile.astype(F32)
        kept.append(tile)
        square = square + jnp.sum(tile * tile, axis=-1, keepdims=True)
    factor = lax.rsqrt(square * (1.0 / D) + EPS)
    for k in range(16):
        tile = (kept[k] * factor * gain[k]).astype(BF)
        for s in range(4):
            normed_ref[s, :, 128 * k : 128 * (k + 1)] = tile


def join_kernel(mine_ref, got_ref, out_ref):
    for s in range(4):
        at = slice(48 * s, 48 * (s + 1))
        out_ref[s] = (mine_ref[at, :].astype(F32) + got_ref[at, :].astype(F32)).astype(BF)


def ffn_kernel(own_ref, other_ref, scale_ref, *refs):
    pieces, (keep_ref, send_ref, hidden_ref) = refs[:8], refs[8:]
    for half, ref in ((0, own_ref), (1, other_ref)):
        for lo in range(0, 1024, 256):
            total = None
            for i, piece in enumerate(pieces):
                part = jnp.dot(
                    ref[:, 256 * i : 256 * (i + 1)],
                    piece[:, lo : lo + 256],
                    preferred_element_type=F32,
                )
                total = part if total is None else total + part
            value = jnp.maximum(total * scale_ref[:, lo : lo + 256], 0.0)
            hidden_ref[half, :, lo : lo + 256] = (value * value).astype(BF)
    for half, ref in ((1, send_ref), (0, keep_ref)):
        for i, piece in enumerate(pieces):
            ref[:, 256 * i : 256 * (i + 1)] = lax.dot_general(
                hidden_ref[half], piece[:, 1024:], NT, preferred_element_type=F32
            ).astype(BF)


def last_kernel(where_ref, parts_ref, residual_ref, out_ref):
    z = where_ref[0]
    for i, d in enumerate(OFFSETS):
        base = pl.multiple_of(((z + d) & 7) * 256, 256)
        at = slice(256 * i, 256 * (i + 1))
        total = parts_ref[0, :, at].astype(F32)
        for s in range(1, 4):
            total = total + parts_ref[s, :, at].astype(F32)
        tile = (residual_ref[:, at].astype(F32) + total).astype(BF)
        for s in range(4):
            out_ref[s, :, pl.ds(base, 256)] = tile


def place_own_kernel(where_ref, own_ref, out_ref, sem):
    half = ROWS // 2
    start = pl.multiple_of(where_ref[2] * half, half)
    copy = pltpu.make_async_copy(own_ref, out_ref.at[pl.ds(start, half), :], sem)
    copy.start()
    copy.wait()


def place_other_kernel(where_ref, other_ref, held_ref, out_ref, sem):
    half = ROWS // 2
    start = pl.multiple_of((1 - where_ref[2]) * half, half)
    copy = pltpu.make_async_copy(other_ref, out_ref.at[pl.ds(start, half), :], sem)
    copy.start()
    copy.wait()


def near(value):
    return pltpu.with_memory_space_constraint(value, pltpu.VMEM)


def call(kernel, outs, scratch, *args):
    vmem = pl.BlockSpec(memory_space=pltpu.VMEM)
    smem = pl.BlockSpec(memory_space=pltpu.SMEM)
    return pl.pallas_call(
        kernel,
        out_shape=[pltpu.VMEM(s, t) for s, t in outs],
        in_specs=[smem if a.dtype == jnp.int32 else vmem for a in args],
        out_specs=[vmem] * len(outs),
        scratch_shapes=[pltpu.VMEM(s, t) for s, t in scratch],
        compiler_params=pltpu.CompilerParams(vmem_limit_bytes=VMEM_LIMIT),
    )(*args)


def place(where, own, other):
    vmem = pl.BlockSpec(memory_space=pltpu.VMEM)
    smem = pl.BlockSpec(memory_space=pltpu.SMEM)
    far = pl.BlockSpec(memory_space=pl.ANY)
    shape = jax.ShapeDtypeStruct((ROWS, D), BF)
    held = pl.pallas_call(
        place_own_kernel,
        out_shape=shape,
        in_specs=[smem, vmem],
        out_specs=far,
        scratch_shapes=[pltpu.SemaphoreType.DMA],
        compiler_params=pltpu.CompilerParams(vmem_limit_bytes=VMEM_LIMIT),
        name="place_own",
    )(where, near(own))
    return pl.pallas_call(
        place_other_kernel,
        out_shape=shape,
        in_specs=[smem, vmem, far],
        out_specs=far,
        scratch_shapes=[pltpu.SemaphoreType.DMA],
        input_output_aliases={2: 0},
        compiler_params=pltpu.CompilerParams(vmem_limit_bytes=VMEM_LIMIT),
        name="place_other",
    )(where, near(other), held)


def body(
    x,
    pre_gain,
    w_probe,
    s_probe,
    w_lookup,
    s_lookup,
    w_forget,
    s_forget,
    shift,
    burst,
    w_content,
    s_content,
    w_filter,
    s_filter,
    head_gain,
    w_emission,
    s_emission,
    mlp_gain,
    w_raising,
    s_raising,
    w_lowering,
    s_lowering,
):
    fs = lax.axis_index("fs")
    tp = lax.axis_index("tp")
    where = jnp.stack([fs >> 2, fs & 3, tp & 1, tp >> 1]).astype(jnp.int32)
    tables = (
        w_probe,
        w_lookup,
        w_forget,
        w_content,
        w_filter,
        w_emission.T,
        w_raising,
        w_lowering.T,
        s_emission[None, :],
        s_lowering[None, :],
    )
    vmem = pl.BlockSpec(memory_space=pltpu.VMEM)
    far = pl.BlockSpec(memory_space=pl.ANY)
    attention, ffn = pl.pallas_call(
        cast_kernel,
        out_shape=[pltpu.VMEM((64, 1152), BF), pltpu.VMEM((4, 64, 2048), BF)],
        in_specs=[far] * 10,
        out_specs=[vmem] * 2,
        scratch_shapes=[pltpu.VMEM(w.shape, F32) for w in tables]
        + [pltpu.SemaphoreType.DMA((10,))],
        compiler_params=pltpu.CompilerParams(vmem_limit_bytes=VMEM_LIMIT),
        name="cast",
    )(
        *(pltpu.with_memory_space_constraint(w, pltpu.HBM) for w in tables)
    )
    (along_z,) = call(stack_kernel, [((512, 1152), BF)], [], *(near(b) for b in z_mixed(attention)))
    first_tables, second_tables = y_gather(along_z)
    pieces = z_relay(y_exchange(ffn).reshape(256, 2048))

    (normed,) = call(norm_kernel, [((ROWS, D), BF)], [((48, D), F32)], where, x, pre_gain[None, :])
    first_tables = [near(t) for t in first_tables]
    (early,) = call(early_kernel, [((ROWS, 896), F32)], [], near(normed), *first_tables)
    keep, send = call(
        mixing_kernel,
        [((ROWS // 2, D), BF)] * 2,
        [
            ((ROWS, 128), F32),
            ((ROWS, 128), F32),
            ((ROWS, 256), BF),
            ((ROWS, 128), F32),
            ((ROWS, 256), F32),
            ((ROWS, 256), BF),
            ((256, 128), F32),
        ],
        where,
        near(normed),
        near(early),
        *first_tables,
        *(near(t) for t in second_tables),
        s_probe[None, :],
        s_lookup[None, :],
        s_forget[None, :],
        s_content[None, :],
        s_filter[None, :],
        shift[None, :],
        burst.T,
        head_gain[None, :],
    )

    def reduce_rows(keep, send):
        (both,) = call(join_kernel, [((4, 48, D), BF)], [], near(keep), near(core_swap(send)))
        return near(x_exchange(both))

    def spread_rows(copies):
        half = x_exchange(copies).reshape(ROWS // 2, D)
        return half, core_swap(half)

    own_rows = lax.dynamic_slice_in_dim(x, where[2] * 192 + where[3] * 48, 48, 0)
    residual, normed_share = call(
        middle_kernel,
        [((48, D), BF), ((4, 48, D), BF)],
        [],
        where,
        reduce_rows(keep, send),
        own_rows,
        mlp_gain[None, :],
    )
    own, other = spread_rows(normed_share)
    sums = call(
        ffn_kernel,
        [((ROWS // 2, D), BF)] * 2,
        [((2, ROWS // 2, 1024), BF)],
        near(own),
        near(other),
        s_raising[None, :],
        *(near(p) for p in pieces),
    )
    (shares,) = call(last_kernel, [((4, 48, D), BF)], [], where, reduce_rows(*sums), near(residual))
    return place(where, *spread_rows(shares))


def solution(mesh):
    return jax.shard_map(
        body,
        mesh=mesh,
        in_specs=(
            P(("rep", "fs"), None),
            P(),
            P("fs", "tp"),
            P("tp"),
            P("fs", "tp"),
            P("tp"),
            P("fs", "tp"),
            P("tp"),
            P("tp"),
            P(("rep", "fs"), "tp"),
            P("fs", "tp"),
            P("tp"),
            P("fs", "tp"),
            P("tp"),
            P("tp"),
            P("tp", "fs"),
            P("fs"),
            P(),
            P("fs", "tp"),
            P("tp"),
            P("tp", "fs"),
            P("fs"),
        ),
        out_specs=P(("rep", "fs"), None),
        check_vma=False,
    )
```
